32 devices in a mesh: sp: 8 (over z, core), tp: 4 (over y, x).
Axes of the slice: x: 2, y: 2, z: 4, core: 2. Of those that a mesh axis runs over, the one named last changes fastest.
Arguments:
- residual: bfloat16 [1024, 4096], P('sp', 'tp'), may hold values from -46 to 46
- query_small: bfloat16 [1024, 2048], P('sp', 'tp'), may hold values from -6 to 6
- key_narrow_group: bfloat16 [1024, 2048], P('sp', 'tp'), may hold values from -6 to 6
- query_large: bfloat16 [1024, 4096], P('sp', 'tp'), may hold values from -6 to 6
- key_large: bfloat16 [1024, 4096], P('sp', 'tp'), may hold values from -6 to 6
- values: bfloat16 [1024, 2, 2048], P('sp', None, 'tp'), may hold values from -6 to 6
- gates: bfloat16 [1024, 2, 2048], P('sp', None, 'tp'), may hold values from -6 to 6
- log_decay: float32 [1024, 2, 16], P('sp', None, 'tp'), may hold values from -0.65 to 0, as said below
- head_gain: float32 [2, 2048], P(None, 'tp'), may hold values from 0.1 to 1.9
- out_weight: bfloat16 [2, 2048, 4096], P(None, 'sp', 'tp'), may hold values from -0.09375 to 0.09375
- norm_gain: float32 [4096], P('tp'), may hold values from 0.1 to 1.9
- routes: int32 [1024, 2], P('sp'), may hold values from 0 to 7, all different within a row; in each aligned block of 128 rows (0 to 127, 128 to 255, ...) at most 64 rows name the same one
- route_weight: float32 [1024, 2], P('sp'), may hold values from 0.2 to 1
- expert_gate: bfloat16 [8, 4096, 2048], P('sp', None, 'tp'), may hold values from -0.09375 to 0.09375
- expert_up: bfloat16 [8, 4096, 2048], P('sp', None, 'tp'), may hold values from -0.09375 to 0.09375
- expert_down: bfloat16 [8, 2048, 4096], P('sp', None, 'tp'), may hold values from -0.5 to 0.5
Outputs:
- new_stream: bfloat16 [1024, 4096], P('sp', 'tp')
The draws below stay inside these ranges and needn't reach their ends.
Inputs may be any that keep to these rules, and one draw needn't show every extreme that they name: `routes`: each row names two different experts; in each aligned block of 128 rows no expert is named more than 64 times, a bound that some block reaches. `log_decay`: negative at every position.
All inputs are finite; a program needn't handle non-finite values.
Results may differ from the reference program's by a relative error of at most 0.019.
Values may be sent and summed in bfloat16 or wider, within the bound.
A program may use at most 64 MiB of HBM per device.

```python
import math
import jax
import jax.numpy as jnp
import numpy as np
from jax import lax

D = 4096
H = 16
DKA = 128
DKB = 256
DV = 128
FF = 2048
TOK_DEV = 128
TOKENS = 1024
EXPERTS = 8
CAP = 64
N_SP = 8


def draw_residual(key, part):
    keys = jax.random.split(key, 3)
    base = jnp.clip(jax.random.normal(keys[0], (TOKENS, D), jnp.float32), -5.0, 5.0)
    ramp = jnp.arange(D, dtype=jnp.float32) / D
    coarse_estimate = jax.random.uniform(keys[1], (1, D), jnp.float32, 0.5, 1.5)
    columns = 0.3 * jnp.power(10.0, ramp)
    row_scale = jnp.exp(jax.random.uniform(keys[2], (TOKENS, 1), jnp.float32, -0.7, 0.7))
    return (base * columns[None, :] * coarse_estimate * row_scale).astype(jnp.bfloat16)


def draw_log_decay(key, part):
    keys = jax.random.split(key, 7)
    choose = jax.random.uniform(keys[0], (1, 2, H), jnp.float32)
    slow_heads = choose < 0.5
    fast_rate = jnp.exp(-jax.random.uniform(keys[1], (1, 2, H), jnp.float32, 3.4, 4.1))
    slow_rate = jax.random.uniform(keys[2], (1, 2, H), jnp.float32, 0.1, 0.4) / TOKENS
    decay_speed = jnp.where(slow_heads, slow_rate, fast_rate)
    block_count = TOKENS // TOK_DEV
    multiplier_term = jnp.exp(jax.random.uniform(keys[3], (block_count, 1, 1), jnp.float32, -0.69, 0.69))
    multiplier_term = jnp.repeat(multiplier_term, TOK_DEV, axis=0)
    coarse_estimate = jax.random.uniform(keys[4], (TOKENS, 2, H), jnp.float32, 0.5, 1.5)
    spots = jax.random.randint(keys[5], (3,), 0, TOKENS)
    hit_marker = jnp.any(jnp.arange(TOKENS)[:, None] == spots[None, :], axis=1)
    kept_fraction = jax.random.uniform(keys[6], (TOKENS, 1, 1), jnp.float32, 0.6, 0.8)
    spike_amount = jnp.where(hit_marker[:, None, None], jnp.log(kept_fraction), 0.0)
    return (-decay_speed * multiplier_term * coarse_estimate + spike_amount).astype(jnp.float32)


def levels(stream_key, shape, cuts, smallest, high):
    def one(dim, parts):
        draws = jax.random.uniform(jax.random.fold_in(jax.random.fold_in(stream_key, 6), dim), (parts,), jnp.float32, smallest / len(cuts), high / len(cuts))
        return jnp.repeat(jnp.exp(draws), shape[dim] // parts).reshape((-1,) + (1,) * (len(shape) - dim - 1))

    level = one(*cuts[0])
    for cut in cuts[1:]:
        level = level * one(*cut)
    return level


def shared_out(rng, own, number, rows, count, top, reach, slope):
    order = jax.random.permutation(rng, count)
    packed, usual = portions_of(count, rows * top, reach, slope, True), portions_of(count, rows * top, reach, slope, False)
    places = jnp.arange(count)

    def named(lengths, rotation):
        used = int((lengths > 0).sum())
        fixed = max(1, used // 4)
        moved = fixed + (places - fixed + rotation * (used - fixed)) % max(1, count - fixed)
        return jnp.zeros((count,), jnp.int32).at[order[jnp.where(places < fixed, places, moved)]].set(jnp.asarray(lengths, jnp.int32))

    lengths = jnp.where(number % 4 == 0, named(packed, number // 4), named(usual, number - number // 4 - 1))
    mixed = jax.random.permutation(jax.random.fold_in(own, 3), count)
    donor, sink = mixed[0:count // 2 * 2:2], mixed[1:count // 2 * 2:2]
    margin = jnp.minimum(lengths[donor] - 1, reach - lengths[sink]) // 2
    margin = jnp.where((donor == order[0]) | (sink == order[0]) | (lengths[sink] == 0), 0, jnp.maximum(margin, 0))
    moved = jax.random.randint(jax.random.fold_in(own, 4), (count // 2,), 0, 1 << 20) % (margin + 1)
    lengths = lengths.at[donor].add(-moved).at[sink].add(moved)
    items = jnp.searchsorted(jnp.cumsum(lengths), jnp.arange(rows * top), side="right").astype(jnp.int32)
    listing = items.reshape(top, rows).T
    listing = listing[jax.random.permutation(jax.random.fold_in(own, 1), rows)]
    rotation = jax.random.randint(jax.random.fold_in(own, 2), (rows, 1), 0, top)
    return jnp.take_along_axis(listing, (jnp.arange(top)[None, :] + rotation) % top, axis=1)


def portions_of(amount, total, reach, skew, full):
    weights = [(1 << 20) // math.isqrt(grade ** skew) + 1 for grade in range(1, amount + 1)]
    largest = reach if full else min(reach, max(-(-total // amount), total * weights[0] // sum(weights)))
    least = 1 if total - largest >= amount - 1 else 0
    given, spare = [largest] + [least] * (amount - 1), total - largest - least * (amount - 1)
    while spare > 0:
        candidates = [i for i in range(1, amount) if given[i] < largest] or [i for i in range(1, amount) if given[i] < reach]
        whole, left = sum([weights[i] for i in candidates]), spare
        for i in candidates:
            extra = min(reach - given[i], max(1, left * weights[i] // whole), spare)
            given[i] = given[i] + extra
            spare = spare - extra
    return np.array(given)


def scatter_about(own_key, dims, scale, most, cuts=(), held_as=jnp.bfloat16):
    result = jax.random.normal(own_key, dims, jnp.float32) * scale
    if len(cuts) > 0:
        result = levels(own_key, dims, cuts, -0.22, 0.18) * result
    return jnp.clip(result, min=-most, max=most).astype(held_as)


def setup_inputs(seed: int = 0) -> dict:
    key_of = jax.random.split(jax.random.key(seed), 17)
    residual = draw_residual(jax.random.fold_in(key_of[16], 71), 0)
    query_small = scatter_about(key_of[1], (TOKENS, H * DKA), 1.0, 6.0, ((0, 8), (1, 4)))
    key_narrow_group = scatter_about(key_of[2], (TOKENS, H * DKA), 1.0, 6.0, ((0, 8), (1, 4)))
    query_large = scatter_about(key_of[3], (TOKENS, H * DKB), 1.0, 6.0, ((0, 8), (1, 4)))
    key_large = scatter_about(key_of[4], (TOKENS, H * DKB), 1.0, 6.0, ((0, 8), (1, 4)))
    values = scatter_about(key_of[5], (TOKENS, 2, H * DV), 1.0, 6.0, ((0, 8), (2, 4)))
    gates = scatter_about(key_of[6], (TOKENS, 2, H * DV), 1.0, 6.0, ((0, 8), (2, 4)))
    log_decay = draw_log_decay(jax.random.fold_in(key_of[16], 71), 0)
    head_gain = jnp.clip(1.0 + 0.18 * jax.random.normal(key_of[8], (2, H * DV), jnp.float32), 0.1, 1.9)
    out_weight = scatter_about(key_of[9], (2, H * DV, D), (2 * H * DV) ** -0.5, 0.09375, ((1, 8), (2, 4)))
    norm_gain = jnp.clip(1.0 + 0.18 * jax.random.normal(key_of[10], (D,), jnp.float32), 0.1, 1.9)
    routes_keys = jax.random.split(jax.random.fold_in(key_of[11], 1), TOKENS // TOK_DEV)
    routes_turns = jax.random.permutation(jax.random.fold_in(key_of[11], 3), TOKENS // TOK_DEV)
    routes = jax.vmap(lambda own, number: shared_out(jax.random.fold_in(key_of[11], 2), own, number, TOK_DEV, EXPERTS, 2, CAP, 2))(routes_keys, routes_turns).reshape((TOKENS, 2))
    route_weight = jnp.clip(0.2 + 0.8 * jax.random.uniform(key_of[12], (TOKENS, 2), jnp.float32) ** levels(key_of[12], (TOKENS, 2), ((0, 8),), -0.2, 0.2), 0.2, 1.0)
    expert_gate = scatter_about(key_of[13], (EXPERTS, D, FF), D ** -0.5, 0.09375, ((0, 8), (2, 4)))
    expert_up = scatter_about(key_of[14], (EXPERTS, D, FF), D ** -0.5, 0.09375, ((0, 8), (2, 4)))
    expert_down = scatter_about(key_of[15], (EXPERTS, FF, D), (FF // 16) ** -0.5, 0.5, ((0, 8), (2, 4)))
    return {"residual": residual, "query_small": query_small, "key_narrow_group": key_narrow_group, "query_large": query_large, "key_large": key_large, "values": values, "gates": gates, "log_decay": log_decay, "head_gain": head_gain, "out_weight": out_weight, "norm_gain": norm_gain, "routes": routes, "route_weight": route_weight, "expert_gate": expert_gate, "expert_up": expert_up, "expert_down": expert_down}


EPS = 1e-06
THETA = 10000.0

def rotate(block, positions):
    half_dim = block.shape[-1] // 2
    inverse = jnp.power(THETA, -jnp.arange(half_dim, dtype=jnp.float32) * 2.0 / block.shape[-1])
    angles = positions[:, None, None] * inverse
    cosine_val, sine_val = (jnp.cos(angles), jnp.sin(angles))
    lower_half, upper_half = (block[..., :half_dim], block[..., half_dim:])
    return jnp.concatenate([lower_half * cosine_val - upper_half * sine_val, upper_half * cosine_val + lower_half * sine_val], axis=-1)

def block_terms(rot_queries, rot_keys, value_heads, rates):
    count = rates.shape[0]
    decay_sum = jnp.cumsum(rates, axis=0)
    by_head = decay_sum.T
    causal = (jnp.arange(count)[:, None] >= jnp.arange(count)[None, :])[None]
    spread = by_head[:, :, None] - by_head[:, None, :]
    weight = jnp.where(causal, jnp.exp(jnp.where(causal, spread, 0.0)), 0.0)
    scores = jnp.einsum('ihd,jhd->hij', rot_queries.astype(jnp.float32), rot_keys.astype(jnp.float32))
    weighted = (scores * weight).astype(jnp.bfloat16)
    within = jnp.einsum('hij,jhv->ihv', weighted.astype(jnp.float32), value_heads.astype(jnp.float32))
    block_end = decay_sum[-1]
    carried = (rot_keys.astype(jnp.float32) * jnp.exp(block_end[None, :] - decay_sum)[:, :, None]).astype(jnp.bfloat16)
    update = jnp.einsum('jhd,jhv->hdv', carried.astype(jnp.float32), value_heads.astype(jnp.float32))
    return (within, decay_sum, jnp.exp(block_end), update)

def final_result(rot_queries, decay_sum, within, state_in, gate_part, gain_part):
    cross_part = jnp.einsum('ihd,hdv->ihv', rot_queries.astype(jnp.float32), state_in, precision=lax.Precision.HIGHEST) * jnp.exp(decay_sum)[:, :, None]
    retained = within + cross_part
    scaled = retained * lax.rsqrt(lax.optimization_barrier(jnp.mean(retained * retained, axis=-1, keepdims=True)) + EPS)
    count, head_count, value_size = retained.shape
    gated = jax.nn.silu(gate_part.astype(jnp.float32)).reshape(count, head_count, value_size)
    return (scaled * gain_part.reshape(head_count, value_size) * gated).reshape(count, -1).astype(jnp.bfloat16)

def group_out(queries, keys_in, value_part, gate_part, rates, gain_part, key_size):
    length = queries.shape[0]
    head_count = rates.shape[1]
    value_size = value_part.shape[1] // head_count
    positions = jnp.arange(length, dtype=jnp.float32)
    rot_queries = rotate(queries.astype(jnp.float32).reshape(length, head_count, key_size), positions).astype(jnp.bfloat16)
    rot_keys = (rotate(keys_in.astype(jnp.float32).reshape(length, head_count, key_size), positions) * key_size ** (-0.5)).astype(jnp.bfloat16)
    value_heads = value_part.reshape(length, head_count, value_size)
    block_count = length // TOK_DEV

    def split_blocks(array):
        return array.reshape((block_count, TOK_DEV) + array.shape[1:])

    def advance(state, inputs):
        block_q, block_k, block_v, block_rates, block_gate = inputs
        within, decay_sum, fall, update = block_terms(block_q, block_k, block_v, block_rates)
        output = final_result(block_q, decay_sum, within, state, block_gate, gain_part)
        return (fall[:, None, None] * state + update, output)
    start_state = jnp.zeros((head_count, key_size, value_size), jnp.float32)
    _, outputs = lax.scan(advance, start_state, (split_blocks(rot_queries), split_blocks(rot_keys), split_blocks(value_heads), split_blocks(rates), split_blocks(gate_part)))
    return outputs.reshape(length, head_count * value_size)

def reference(residual, query_small, key_narrow_group, query_large, key_large, values, gates, log_decay, head_gain, out_weight, norm_gain, routes, route_weight, expert_gate, expert_up, expert_down):
    out_small = group_out(query_small, key_narrow_group, values[:, 0], gates[:, 0], log_decay[:, 0], head_gain[0], DKA)
    out_large = group_out(query_large, key_large, values[:, 1], gates[:, 1], log_decay[:, 1], head_gain[1], DKB)
    mixed = (jnp.dot(out_small, out_weight[0], preferred_element_type=jnp.float32) + jnp.dot(out_large, out_weight[1], preferred_element_type=jnp.float32)).astype(jnp.bfloat16)
    stream = residual.astype(jnp.float32) + mixed.astype(jnp.float32)
    normed = (stream * lax.rsqrt(lax.optimization_barrier(jnp.mean(stream * stream, axis=-1, keepdims=True)) + EPS) * norm_gain[None, :]).astype(jnp.bfloat16)
    experts = N_SP
    capacity = 4 * TOK_DEV // experts
    one_hot = (routes[:, :, None] == jnp.arange(experts, dtype=jnp.int32)[None, None, :]).astype(jnp.int32)
    one_hot = one_hot.reshape(N_SP, 2 * TOK_DEV, experts)
    before = jnp.cumsum(one_hot, axis=1) - one_hot
    slot_index = lax.optimization_barrier(jnp.sum(before * one_hot, axis=2)).reshape(TOKENS, 2)
    block_index = (jnp.arange(TOKENS, dtype=jnp.int32) // TOK_DEV).astype(jnp.int32)
    row_slot = (block_index[:, None] * capacity + slot_index).astype(jnp.int32)
    buffer = jnp.zeros((experts, N_SP * capacity, D), jnp.bfloat16)
    buffer = buffer.at[routes, row_slot].set(jnp.broadcast_to(normed[:, None, :], (TOKENS, 2, D)))

    def apply_expert(operands):
        rows_in, w_gate, w_up, w_down = operands
        gate_part = jnp.dot(rows_in, w_gate, preferred_element_type=jnp.float32)
        up_part = jnp.dot(rows_in, w_up, preferred_element_type=jnp.float32)
        hidden = (jax.nn.silu(gate_part) * up_part).astype(jnp.bfloat16)
        return jnp.dot(hidden, w_down, preferred_element_type=jnp.float32).astype(jnp.bfloat16)
    results = lax.map(apply_expert, (buffer, expert_gate, expert_up, expert_down))
    first_pick = results[routes[:, 0], row_slot[:, 0]].astype(jnp.float32)
    second_pick = results[routes[:, 1], row_slot[:, 1]].astype(jnp.float32)
    routed = route_weight[:, 0:1] * first_pick + route_weight[:, 1:2] * second_pick
    return (stream + routed).astype(jnp.bfloat16)
```

```python
import jax
import jax.numpy as jnp
from jax import lax
from jax.experimental import pallas as pl
from jax.experimental.pallas import tpu as pltpu
from jax.sharding import PartitionSpec as P

MESH = pl.DeviceIdType.MESH


EPS = 1e-06
THETA = 10000.0


def greet(axes):
    barrier = pltpu.get_barrier_semaphore()
    total = 0
    for axis in axes:
        count, me = lax.axis_size(axis), lax.axis_index(axis)

        def signal(k, _, axis=axis, count=count, me=me):
            pl.semaphore_signal(
                barrier, inc=1, device_id={axis: (me + k) % count}, device_id_type=MESH
            )
            return 0

        lax.fori_loop(1, count, signal, 0)
        total += count - 1
    pl.semaphore_wait(barrier, total)


def remote(source, target, send_sem, recv_sem, axis, index):
    return pltpu.make_async_remote_copy(
        src_ref=source,
        dst_ref=target,
        send_sem=send_sem,
        recv_sem=recv_sem,
        device_id={axis: index},
        device_id_type=MESH,
    )


def chain_kernel(update_ref, fall_ref, out_ref, held, outgoing, send_sem, recv_sem):
    count, me = lax.axis_size("sp"), lax.axis_index("sp")
    pieces = update_ref.shape[0]
    right, left = (me + 1) % count, (me + count - 1) % count
    barrier = pltpu.get_barrier_semaphore()
    for neighbour in (left, right):
        pl.semaphore_signal(barrier, inc=1, device_id={"sp": neighbour}, device_id_type=MESH)
    pl.semaphore_wait(barrier, 2)

    def hop(c):
        return remote(
            outgoing.at[c], held.at[c], send_sem.at[c], recv_sem.at[c], "sp", right
        )

    def step(c, _):
        @pl.when(me == 0)
        def _():
            held[c] = jnp.zeros(held.shape[1:], held.dtype)

        @pl.when(me > 0)
        def _():
            hop(c).wait_recv()

        @pl.when(me < count - 1)
        def _():
            outgoing[c] = (fall_ref[c] * held[c].astype(jnp.float32) + update_ref[c]).astype(
                outgoing.dtype
            )
            hop(c).start()

        out_ref[c] = held[c]
        return 0

    lax.fori_loop(0, pieces, step, 0)

    @pl.when(me < count - 1)
    def _():
        def finish(c, _):
            hop(c).wait_send()
            return 0

        lax.fori_loop(0, pieces, finish, 0)


def entering_states(update, fall):
    pieces, rows, columns = update.shape
    return pl.pallas_call(
        chain_kernel,
        out_shape=jax.ShapeDtypeStruct(update.shape, jnp.bfloat16),
        in_specs=[pl.BlockSpec(memory_space=pltpu.VMEM)] * 2,
        out_specs=pl.BlockSpec(memory_space=pltpu.VMEM),
        scratch_shapes=[
            pltpu.VMEM((pieces, rows, columns), jnp.bfloat16),
            pltpu.VMEM((pieces, rows, columns), jnp.bfloat16),
            pltpu.SemaphoreType.DMA((pieces,)),
            pltpu.SemaphoreType.DMA((pieces,)),
        ],
        compiler_params=pltpu.CompilerParams(collective_id=0, has_side_effects=True),
    )(update, fall)


def gather_kernel(part_ref, out_ref, held, send_sem, recv_sem):
    count, me = lax.axis_size("tp"), lax.axis_index("tp")
    width = part_ref.shape[2]
    greet(("tp",))

    def place(index):
        return held.at[:, :, pl.ds(pl.multiple_of(index * width, width), width)]

    def start(k, _):
        remote(part_ref, place(me), send_sem.at[k], recv_sem.at[me], "tp", (me + k) % count).start()
        return 0

    lax.fori_loop(1, count, start, 0)
    held[:, :, pl.ds(pl.multiple_of(me * width, width), width)] = part_ref[...]

    def finish(k, _):
        other = (me + k) % count
        remote(part_ref, place(other), send_sem.at[k], recv_sem.at[other], "tp", other).wait()
        return 0

    lax.fori_loop(1, count, finish, 0)
    out_ref[...] = held[...]


def gather_heads(part, count):
    whole = part.shape[:2] + (part.shape[2] * count,)
    return pl.pallas_call(
        gather_kernel,
        out_shape=jax.ShapeDtypeStruct(whole, part.dtype),
        in_specs=[pl.BlockSpec(memory_space=pltpu.VMEM)],
        out_specs=pl.BlockSpec(memory_space=pltpu.VMEM),
        scratch_shapes=[
            pltpu.VMEM(whole, part.dtype),
            pltpu.SemaphoreType.DMA((count,)),
            pltpu.SemaphoreType.DMA((count,)),
        ],
        compiler_params=pltpu.CompilerParams(collective_id=1, has_side_effects=True),
    )(part)


def experts_kernel(
    stream_ref,
    gain_ref,
    select_ref,
    gate_hbm,
    up_hbm,
    down_hbm,
    out_ref,
    w_gate,
    w_up,
    w_down,
    squares,
    outgoing,
    arrived,
    hidden,
    result,
    returned,
    acc_a,
    acc_b,
    acc_c,
    load_sem,
    sq_send,
    sq_recv,
    disp_send,
    disp_recv,
    fwd_send,
    fwd_recv,
    hid_send,
    hid_recv,
    ret_send,
    ret_recv,
):
    n_sp, n_tp = lax.axis_size("sp"), lax.axis_size("tp")
    s, t = lax.axis_index("sp"), lax.axis_index("tp")
    half = n_sp // 2
    cap = outgoing.shape[0] // n_sp
    cols = stream_ref.shape[1]
    units = w_gate.shape[1]
    loads = [
        pltpu.make_async_copy(source.at[0], target, load_sem.at[i])
        for i, (source, target) in enumerate(
            ((gate_hbm, w_gate), (up_hbm, w_up), (down_hbm, w_down))
        )
    ]
    for load in loads:
        load.start()
    greet(("sp", "tp"))

    def rows_of(p):
        return pl.ds(pl.multiple_of(p * cap, cap), cap)

    def group_base(g):
        return ((s // half + g) % 2) * half

    def group_rows(g):
        return pl.ds(pl.multiple_of(group_base(g) * cap, half * cap), half * cap)

    stream = stream_ref[...]
    own = jnp.sum(stream * stream, axis=1, keepdims=True)
    squares[t] = jnp.broadcast_to(own, squares.shape[1:])

    def square_copy(k, source):
        block, other = squares.at[source], (t + k) % n_tp
        return remote(block, block, sq_send.at[k], sq_recv.at[source], "tp", other)

    def square_start(k, _):
        square_copy(k, t).start()
        return 0

    def square_wait(k, _):
        square_copy(k, (t + k) % n_tp).wait()
        return 0

    lax.fori_loop(1, n_tp, square_start, 0)
    lax.fori_loop(1, n_tp, square_wait, 0)
    total = squares[0]
    for p in range(1, n_tp):
        total = total + squares[p]
    scale = lax.rsqrt(total[:, 0:1] / (cols * n_tp) + EPS)
    normed = (stream_ref[...] * scale * gain_ref[...]).astype(jnp.bfloat16)
    outgoing[...] = jnp.dot(
        select_ref[...], normed, preferred_element_type=jnp.float32
    ).astype(jnp.bfloat16)

    def dispatch(p, q):
        return remote(
            outgoing.at[rows_of(p)],
            arrived.at[t, rows_of(q)],
            disp_send.at[p],
            disp_recv.at[q],
            "sp",
            p,
        )

    def others(g, action):
        def body(j, _):
            p = group_base(g) + (s + j) % half

            @pl.when(p != s)
            def _():
                action(p)

            return 0

        lax.fori_loop(0, half, body, 0)

    for g in range(2):
        others(g, lambda p: dispatch(p, s).start())
    arrived[t, rows_of(s)] = outgoing[rows_of(s)]

    def forward(g):
        def body(j, _):
            p = group_base(g) + (s + j) % half

            @pl.when(p != s)
            def _():
                dispatch(p, p).wait_recv()

            def send(k, _):
                block = arrived.at[t, rows_of(p)]
                remote(
                    block, block, fwd_send.at[g, k], fwd_recv.at[g, t], "tp", (t + k) % n_tp
                ).start()
                return 0

            lax.fori_loop(1, n_tp, send, 0)
            return 0

        lax.fori_loop(0, half, body, 0)

    def forwarded(g, k):
        other = (t + k) % n_tp
        block = arrived.at[other, group_rows(g)]
        return remote(block, block, fwd_send.at[g, k], fwd_recv.at[g, other], "tp", other)

    def hidden_copy(g, k, source):
        block = hidden.at[source, group_rows(g)]
        return remote(
            block, block, hid_send.at[g, k], hid_recv.at[g, source], "tp", (t + k) % n_tp
        )

    for g in range(2):
        forward(g)
    for load in loads:
        load.wait()

    def through_units(g):
        acc_a[...] = jnp.zeros_like(acc_a)
        acc_b[...] = jnp.zeros_like(acc_b)

        def body(k, _):
            @pl.when(k > 0)
            def _():
                forwarded(g, k).wait_recv()

            p = (t + k) % n_tp
            part = pl.ds(pl.multiple_of(p * cols, cols), cols)
            rows = arrived[p, group_rows(g)]
            acc_a[...] += jnp.dot(rows, w_gate[part, :], preferred_element_type=jnp.float32)
            acc_b[...] += jnp.dot(rows, w_up[part, :], preferred_element_type=jnp.float32)
            return 0

        lax.fori_loop(0, n_tp, body, 0)
        hidden[t, group_rows(g)] = (jax.nn.silu(acc_a[...]) * acc_b[...]).astype(jnp.bfloat16)

        def send(k, _):
            hidden_copy(g, k, t).start()
            return 0

        lax.fori_loop(1, n_tp, send, 0)

    def give_back(p, q):
        return remote(
            result.at[rows_of(p)], returned.at[rows_of(q)], ret_send.at[p], ret_recv.at[q], "sp", p
        )

    def through_down(g):
        acc_c[...] = jnp.zeros_like(acc_c)

        def body(k, _):
            p = (t + k) % n_tp

            @pl.when(k > 0)
            def _():
                hidden_copy(g, k, p).wait_recv()

            part = pl.ds(pl.multiple_of(p * units, units), units)
            acc_c[...] += jnp.dot(
                hidden[p, group_rows(g)], w_down[part, :], preferred_element_type=jnp.float32
            )
            return 0

        lax.fori_loop(0, n_tp, body, 0)
        result[group_rows(g)] = acc_c[...].astype(jnp.bfloat16)
        others(g, lambda p: give_back(p, s).start())

    for g in ORDER:
        through_units(g)
    for g in ORDER:
        through_down(g)
    returned[rows_of(s)] = result[rows_of(s)]
    for g in range(2):
        others(g, lambda p: give_back(p, p).wait_recv())
    out_ref[...] = returned[...]
    for g in range(2):
        others(g, lambda p: dispatch(p, s).wait_send())
        others(g, lambda p: give_back(p, s).wait_send())

        def finish(k, _, g=g):
            forwarded(g, k).wait_send()
            hidden_copy(g, k, t).wait_send()
            return 0

        lax.fori_loop(1, n_tp, finish, 0)


ORDER = (0, 1)


def through_experts(stream, gain, select, w_gate, w_up, w_down, n_sp, n_tp):
    count, cols = stream.shape
    slots = select.shape[0]
    width, units = w_gate.shape[1:]
    bf16, f32 = jnp.bfloat16, jnp.float32
    dma = pltpu.SemaphoreType.DMA
    vmem = pl.BlockSpec(memory_space=pltpu.VMEM)
    hbm = pl.BlockSpec(memory_space=pl.ANY)
    return pl.pallas_call(
        experts_kernel,
        out_shape=jax.ShapeDtypeStruct((slots, cols), bf16),
        in_specs=[vmem] * 3 + [hbm] * 3,
        out_specs=vmem,
        scratch_shapes=[
            pltpu.VMEM((width, units), bf16),
            pltpu.VMEM((width, units), bf16),
            pltpu.VMEM(w_down.shape[1:], bf16),
            pltpu.VMEM((n_tp, count, 128), f32),
            pltpu.VMEM((slots, cols), bf16),
            pltpu.VMEM((n_tp, slots, cols), bf16),
            pltpu.VMEM((n_tp, slots, units), bf16),
            pltpu.VMEM((slots, cols), bf16),
            pltpu.VMEM((slots, cols), bf16),
            pltpu.VMEM((slots // 2, units), f32),
            pltpu.VMEM((slots // 2, units), f32),
            pltpu.VMEM((slots // 2, cols), f32),
            dma((3,)),
            dma((n_tp,)),
            dma((n_tp,)),
            dma((n_sp,)),
            dma((n_sp,)),
            dma((2, n_tp)),
            dma((2, n_tp)),
            dma((2, n_tp)),
            dma((2, n_tp)),
            dma((n_sp,)),
            dma((n_sp,)),
        ],
        compiler_params=pltpu.CompilerParams(
            collective_id=2, has_side_effects=True, vmem_limit_bytes=50 * 2**20
        ),
    )(stream, gain, select, w_gate, w_up, w_down)


def rotate(block, positions):
    half_dim = block.shape[-1] // 2
    inverse = jnp.power(THETA, -jnp.arange(half_dim, dtype=jnp.float32) * 2.0 / block.shape[-1])
    angles = positions[:, None, None] * inverse
    cosine_val, sine_val = (jnp.cos(angles), jnp.sin(angles))
    lower_half, upper_half = (block[..., :half_dim], block[..., half_dim:])
    return jnp.concatenate(
        [
            lower_half * cosine_val - upper_half * sine_val,
            upper_half * cosine_val + lower_half * sine_val,
        ],
        axis=-1,
    )


def block_terms(rot_queries, rot_keys, value_heads, rates):
    count = rates.shape[0]
    decay_sum = jnp.cumsum(rates, axis=0)
    by_head = decay_sum.T
    causal = (jnp.arange(count)[:, None] >= jnp.arange(count)[None, :])[None]
    spread = by_head[:, :, None] - by_head[:, None, :]
    weight = jnp.where(causal, jnp.exp(jnp.where(causal, spread, 0.0)), 0.0)
    scores = jnp.einsum("ihd,jhd->hij", rot_queries, rot_keys, preferred_element_type=jnp.float32)
    weighted = (scores * weight).astype(jnp.bfloat16)
    within = jnp.einsum("hij,jhv->ihv", weighted, value_heads, preferred_element_type=jnp.float32)
    block_end = decay_sum[-1]
    carried = (
        rot_keys.astype(jnp.float32) * jnp.exp(block_end[None, :] - decay_sum)[:, :, None]
    ).astype(jnp.bfloat16)
    update = jnp.einsum("jhd,jhv->hdv", carried, value_heads, preferred_element_type=jnp.float32)
    return (within, decay_sum, jnp.exp(block_end), update)


def final_result(rot_queries, decay_sum, within, state_in, gate_part, gain_part):
    cross_part = (
        jnp.einsum(
            "ihd,hdv->ihv",
            rot_queries,
            state_in,
            preferred_element_type=jnp.float32,
        )
        * jnp.exp(decay_sum)[:, :, None]
    )
    retained = within + cross_part
    scaled = retained * lax.rsqrt(jnp.mean(retained * retained, axis=-1, keepdims=True) + EPS)
    count, head_count, value_size = retained.shape
    gated = jax.nn.silu(gate_part.astype(jnp.float32)).reshape(count, head_count, value_size)
    return (
        (scaled * gain_part.reshape(head_count, value_size) * gated)
        .reshape(count, -1)
        .astype(jnp.bfloat16)
    )


def prepare(queries, keys_in, value_part, positions, head_count):
    row_count = queries.shape[0]
    key_size = queries.shape[1] // head_count
    rot_queries = rotate(
        queries.astype(jnp.float32).reshape(row_count, head_count, key_size), positions
    ).astype(jnp.bfloat16)
    rot_keys = (
        rotate(keys_in.astype(jnp.float32).reshape(row_count, head_count, key_size), positions)
        * key_size ** (-0.5)
    ).astype(jnp.bfloat16)
    value_heads = value_part.reshape(row_count, head_count, value_part.shape[1] // head_count)
    return (rot_queries, rot_keys, value_heads)


def per_device(
    residual,
    query_small,
    key_narrow_group,
    query_large,
    key_large,
    values,
    gates,
    log_decay,
    head_gain,
    out_weight,
    norm_gain,
    routes,
    route_weight,
    expert_gate,
    expert_up,
    expert_down,
):
    row_count = residual.shape[0]
    head_count = log_decay.shape[2]
    positions = (lax.axis_index("sp") * row_count + jnp.arange(row_count, dtype=jnp.int32)).astype(
        jnp.float32
    )
    query_a, key_a, value_a = prepare(
        query_small, key_narrow_group, values[:, 0], positions, head_count
    )
    query_b, key_b, value_b = prepare(query_large, key_large, values[:, 1], positions, head_count)
    within_a, decay_sum_a, fall_a, update_a = block_terms(query_a, key_a, value_a, log_decay[:, 0])
    within_b, decay_sum_b, fall_b, update_b = block_terms(query_b, key_b, value_b, log_decay[:, 1])

    n_sp, n_tp = lax.axis_size("sp"), lax.axis_size("tp")
    value_size = update_a.shape[2]
    piece = update_a.shape[1]
    parts = update_b.shape[1] // piece
    update = jnp.concatenate([update_a, update_b.reshape(-1, piece, value_size)], axis=0)
    fall = jnp.concatenate([fall_a, jnp.repeat(fall_b, parts)])
    fall = jnp.broadcast_to(fall[:, None, None], (fall.shape[0], 1, value_size))
    entering = entering_states(update, fall)
    state_a = entering[:head_count]
    state_b = entering[head_count:].reshape(update_b.shape)
    output_a = final_result(query_a, decay_sum_a, within_a, state_a, gates[:, 0], head_gain[0])
    output_b = final_result(query_b, decay_sum_b, within_b, state_b, gates[:, 1], head_gain[1])
    gathered = gather_heads(jnp.stack([output_a, output_b], axis=0), n_tp)
    weight = lax.all_gather(out_weight, "sp", axis=1, tiled=True)
    mixed = (
        jnp.dot(gathered[0], weight[0], preferred_element_type=jnp.float32)
        + jnp.dot(gathered[1], weight[1], preferred_element_type=jnp.float32)
    ).astype(jnp.bfloat16)
    stream = residual.astype(jnp.float32) + mixed.astype(jnp.float32)
    experts = lax.axis_size("sp")
    capacity = 4 * row_count // experts
    one_hot = (routes[:, :, None] == jnp.arange(experts, dtype=jnp.int32)[None, None, :]).astype(
        jnp.int32
    )
    one_hot = one_hot.reshape(2 * row_count, experts)
    before = jnp.cumsum(one_hot, axis=0) - one_hot
    slot_index = jnp.sum(before * one_hot, axis=1).reshape(row_count, 2)
    target = routes * capacity + slot_index
    slot_ids = jnp.arange(experts * capacity, dtype=jnp.int32)
    choose = target[:, :, None] == slot_ids[None, None, :]
    select = jnp.sum(choose.astype(jnp.int32), axis=1).astype(jnp.bfloat16).T
    returned = through_experts(
        stream, norm_gain[None, :], select, expert_gate, expert_up, expert_down, n_sp, n_tp
    )
    first_pick = jnp.dot(
        choose[:, 0].astype(jnp.bfloat16), returned, preferred_element_type=jnp.float32
    )
    second_pick = jnp.dot(
        choose[:, 1].astype(jnp.bfloat16), returned, preferred_element_type=jnp.float32
    )
    routed = route_weight[:, 0:1] * first_pick + route_weight[:, 1:2] * second_pick
    return (stream + routed).astype(jnp.bfloat16)


def solution(mesh):
    placed = (
        P("sp", "tp"),
        P("sp", "tp"),
        P("sp", "tp"),
        P("sp", "tp"),
        P("sp", "tp"),
        P("sp", None, "tp"),
        P("sp", None, "tp"),
        P("sp", None, "tp"),
        P(None, "tp"),
        P(None, "sp", "tp"),
        P("tp"),
        P("sp", None),
        P("sp", None),
        P("sp", None, "tp"),
        P("sp", None, "tp"),
        P("sp", None, "tp"),
    )
    return jax.shard_map(
        per_device, mesh=mesh, in_specs=placed, out_specs=P("sp", "tp"), check_vma=False
    )
```

```python
import jax
import jax.numpy as jnp
from jax import lax
from jax.experimental import pallas as pl
from jax.experimental.pallas import tpu as pltpu
from jax.sharding import PartitionSpec as P

MESH = pl.DeviceIdType.MESH


EPS = 1e-06
THETA = 10000.0


def greet(axes):
    barrier = pltpu.get_barrier_semaphore()
    total = 0
    for axis in axes:
        count, me = lax.axis_size(axis), lax.axis_index(axis)

        def signal(k, _, axis=axis, count=count, me=me):
            pl.semaphore_signal(
                barrier, inc=1, device_id={axis: (me + k) % count}, device_id_type=MESH
            )
            return 0

        lax.fori_loop(1, count, signal, 0)
        total += count - 1
    pl.semaphore_wait(barrier, total)


def remote(source, target, send_sem, recv_sem, axis, index):
    return pltpu.make_async_remote_copy(
        src_ref=source,
        dst_ref=target,
        send_sem=send_sem,
        recv_sem=recv_sem,
        device_id={axis: index},
        device_id_type=MESH,
    )


def chain_kernel(update_ref, fall_ref, out_ref, held, outgoing, send_sem, recv_sem):
    count, me = lax.axis_size("sp"), lax.axis_index("sp")
    pieces = update_ref.shape[0]
    right, left = (me + 1) % count, (me + count - 1) % count
    barrier = pltpu.get_barrier_semaphore()
    for neighbour in (left, right):
        pl.semaphore_signal(barrier, inc=1, device_id={"sp": neighbour}, device_id_type=MESH)
    pl.semaphore_wait(barrier, 2)

    def hop(c):
        return remote(
            outgoing.at[c], held.at[c], send_sem.at[c], recv_sem.at[c], "sp", right
        )

    def step(c, _):
        @pl.when(me == 0)
        def _():
            held[c] = jnp.zeros(held.shape[1:], held.dtype)

        @pl.when(me > 0)
        def _():
            hop(c).wait_recv()

        @pl.when(me < count - 1)
        def _():
            outgoing[c] = (fall_ref[c] * held[c].astype(jnp.float32) + update_ref[c]).astype(
                outgoing.dtype
            )
            hop(c).start()

        out_ref[c] = held[c]
        return 0

    lax.fori_loop(0, pieces, step, 0)

    @pl.when(me < count - 1)
    def _():
        def finish(c, _):
            hop(c).wait_send()
            return 0

        lax.fori_loop(0, pieces, finish, 0)


def entering_states(update, fall):
    pieces, rows, columns = update.shape
    return pl.pallas_call(
        chain_kernel,
        out_shape=jax.ShapeDtypeStruct(update.shape, jnp.bfloat16),
        in_specs=[pl.BlockSpec(memory_space=pltpu.VMEM)] * 2,
        out_specs=pl.BlockSpec(memory_space=pltpu.VMEM),
        scratch_shapes=[
            pltpu.VMEM((pieces, rows, columns), jnp.bfloat16),
            pltpu.VMEM((pieces, rows, columns), jnp.bfloat16),
            pltpu.SemaphoreType.DMA((pieces,)),
            pltpu.SemaphoreType.DMA((pieces,)),
        ],
        compiler_params=pltpu.CompilerParams(collective_id=0, has_side_effects=True),
    )(update, fall)


def gather_kernel(part_ref, out_ref, held, send_sem, recv_sem):
    count, me = lax.axis_size("tp"), lax.axis_index("tp")
    width = part_ref.shape[2]
    greet(("tp",))

    def place(index):
        return held.at[:, :, pl.ds(pl.multiple_of(index * width, width), width)]

    def start(k, _):
        remote(part_ref, place(me), send_sem.at[k], recv_sem.at[me], "tp", (me + k) % count).start()
        return 0

    lax.fori_loop(1, count, start, 0)
    held[:, :, pl.ds(pl.multiple_of(me * width, width), width)] = part_ref[...]

    def finish(k, _):
        other = (me + k) % count
        remote(part_ref, place(other), send_sem.at[k], recv_sem.at[other], "tp", other).wait()
        return 0

    lax.fori_loop(1, count, finish, 0)
    out_ref[...] = held[...]


def gather_heads(part, count):
    whole = part.shape[:2] + (part.shape[2] * count,)
    return pl.pallas_call(
        gather_kernel,
        out_shape=jax.ShapeDtypeStruct(whole, part.dtype),
        in_specs=[pl.BlockSpec(memory_space=pltpu.VMEM)],
        out_specs=pl.BlockSpec(memory_space=pltpu.VMEM),
        scratch_shapes=[
            pltpu.VMEM(whole, part.dtype),
            pltpu.SemaphoreType.DMA((count,)),
            pltpu.SemaphoreType.DMA((count,)),
        ],
        compiler_params=pltpu.CompilerParams(collective_id=1, has_side_effects=True),
    )(part)


def experts_kernel(
    stream_ref,
    gain_ref,
    select_ref,
    gate_hbm,
    up_hbm,
    down_hbm,
    out_ref,
    w_gate,
    w_up,
    w_down,
    squares,
    outgoing,
    arrived,
    hidden,
    result,
    returned,
    acc_a,
    acc_b,
    acc_c,
    load_sem,
    sq_send,
    sq_recv,
    disp_send,
    disp_recv,
    fwd_send,
    fwd_recv,
    fwd_relay_send,
    fwd_relay_recv,
    hid_send,
    hid_recv,
    hid_relay_send,
    hid_relay_recv,
    ret_send,
    ret_recv,
):
    n_sp, n_tp = lax.axis_size("sp"), lax.axis_size("tp")
    s, t = lax.axis_index("sp"), lax.axis_index("tp")
    per_group = n_sp // GROUPS
    across, down = grid_of(n_tp)
    x, y = t % across, t // across
    cap = outgoing.shape[0] // n_sp
    cols = stream_ref.shape[1]
    units = w_gate.shape[1]
    loads = [
        pltpu.make_async_copy(source.at[0], target, load_sem.at[i])
        for i, (source, target) in enumerate(
            ((gate_hbm, w_gate), (up_hbm, w_up), (down_hbm, w_down))
        )
    ]
    for load in loads:
        load.start()
    greet(("sp", "tp"))

    def rows_of(p):
        return pl.ds(pl.multiple_of(p * cap, cap), cap)

    def group_base(g):
        return ((s // per_group + g) % GROUPS) * per_group

    def group_rows(g, part=None):
        size = per_group * cap
        start = pl.multiple_of(group_base(g) * cap, size)
        if part is None:
            return pl.ds(start, size)
        return pl.ds(pl.multiple_of(start + part * (size // 2), size // 2), size // 2)

    lines = (
        [y * across + (x + k) % across for k in range(1, across)],
        [((y + k) % down) * across + x for k in range(1, down)],
    )
    direct = lines[0] + lines[1]

    stream = stream_ref[...]
    own = jnp.sum(stream * stream, axis=1, keepdims=True)
    squares[t] = jnp.broadcast_to(own, squares.shape[1:])

    def square_copy(k, source):
        block, other = squares.at[source], (t + k) % n_tp
        return remote(block, block, sq_send.at[k], sq_recv.at[source], "tp", other)

    def square_start(k, _):
        square_copy(k, t).start()
        return 0

    def square_wait(k, _):
        square_copy(k, (t + k) % n_tp).wait()
        return 0

    lax.fori_loop(1, n_tp, square_start, 0)
    lax.fori_loop(1, n_tp, square_wait, 0)
    total = squares[0]
    for p in range(1, n_tp):
        total = total + squares[p]
    scale = lax.rsqrt(total[:, 0:1] / (cols * n_tp) + EPS)
    normed = (stream_ref[...] * scale * gain_ref[...]).astype(jnp.bfloat16)
    outgoing[...] = jnp.dot(
        select_ref[...], normed, preferred_element_type=jnp.float32
    ).astype(jnp.bfloat16)

    def dispatch(p, q):
        return remote(
            outgoing.at[rows_of(p)],
            arrived.at[t, rows_of(q)],
            disp_send.at[p],
            disp_recv.at[q],
            "sp",
            p,
        )

    def members(g, action):
        def body(j, _):
            action(group_base(g) + (s + j) % per_group)
            return 0

        lax.fori_loop(0, per_group, body, 0)

    def others(g, action):
        def guarded(p):
            @pl.when(p != s)
            def _():
                action(p)

        members(g, guarded)

    for g in range(GROUPS):
        others(g, lambda p: dispatch(p, s).start())
    arrived[t, rows_of(s)] = outgoing[rows_of(s)]

    def straight(buffer, sems, g, i, source, rows):
        block = buffer.at[source, rows]
        return remote(block, block, sems[0].at[g, i], sems[1].at[g, source], "tp", direct[i])

    def relayed(buffer, sems, g, part, i, source, target):
        block = buffer.at[source, group_rows(g, part)]
        return remote(
            block, block, sems[2].at[g, part, i], sems[3].at[g, source, part], "tp", target
        )

    def relay(buffer, sems, g):
        for part in range(2):
            for k, source in enumerate(lines[part]):
                i = k if part == 0 else len(lines[0]) + k
                straight(buffer, sems, g, i, source, group_rows(g)).wait_recv()
                for j, target in enumerate(lines[1 - part]):
                    relayed(
                        buffer, sems, g, part, k * len(lines[1 - part]) + j, source, target
                    ).start()

    def place_of(k):
        return ((y + k // across) % down) * across + (x + k % across) % across

    def wait_relayed(buffer, sems, g, k):
        @pl.when((k // across) * (k % across) > 0)
        def _():
            source = place_of(k)
            for part in range(2):
                relayed(buffer, sems, g, part, 0, source, source).wait_recv()

    def finish_sends(buffer, sems, g):
        for i in range(len(direct)):
            straight(buffer, sems, g, i, t, group_rows(g)).wait_send()
        for part in range(2):
            for i in range(len(lines[0]) * len(lines[1])):
                relayed(buffer, sems, g, part, i, t, direct[0]).wait_send()

    arrived_sems = (fwd_send, fwd_recv, fwd_relay_send, fwd_relay_recv)
    hidden_sems = (hid_send, hid_recv, hid_relay_send, hid_relay_recv)

    def forward(g):
        def block(p):
            @pl.when(p != s)
            def _():
                dispatch(p, p).wait_recv()

            for i in range(len(direct)):
                straight(arrived, arrived_sems, g, i, t, rows_of(p)).start()

        members(g, block)

    def through_units(g):
        acc_a[...] = jnp.zeros_like(acc_a)
        acc_b[...] = jnp.zeros_like(acc_b)

        def body(k, _):
            wait_relayed(arrived, arrived_sems, g, k)
            p = place_of(k)
            part = pl.ds(pl.multiple_of(p * cols, cols), cols)
            rows = arrived[p, group_rows(g)]
            acc_a[...] += jnp.dot(rows, w_gate[part, :], preferred_element_type=jnp.float32)
            acc_b[...] += jnp.dot(rows, w_up[part, :], preferred_element_type=jnp.float32)
            return 0

        lax.fori_loop(0, n_tp, body, 0)
        hidden[t, group_rows(g)] = (jax.nn.silu(acc_a[...]) * acc_b[...]).astype(jnp.bfloat16)
        for i in range(len(direct)):
            straight(hidden, hidden_sems, g, i, t, group_rows(g)).start()

    def give_back(p, q):
        return remote(
            result.at[rows_of(p)], returned.at[rows_of(q)], ret_send.at[p], ret_recv.at[q], "sp", p
        )

    def through_down(g):
        acc_c[...] = jnp.zeros_like(acc_c)

        def body(k, _):
            wait_relayed(hidden, hidden_sems, g, k)
            p = place_of(k)
            part = pl.ds(pl.multiple_of(p * units, units), units)
            acc_c[...] += jnp.dot(
                hidden[p, group_rows(g)], w_down[part, :], preferred_element_type=jnp.float32
            )
            return 0

        lax.fori_loop(0, n_tp, body, 0)
        result[group_rows(g)] = acc_c[...].astype(jnp.bfloat16)
        others(g, lambda p: give_back(p, s).start())

    for step in range(GROUPS + 4):
        for late, action in enumerate(
            (
                forward,
                lambda g: relay(arrived, arrived_sems, g),
                through_units,
                lambda g: relay(hidden, hidden_sems, g),
                through_down,
            )
        ):
            if 0 <= step - late < GROUPS:
                if late == 2 and step == 2:
                    for load in loads:
                        load.wait()
                action(step - late)
    returned[rows_of(s)] = result[rows_of(s)]
    for g in range(GROUPS):
        others(g, lambda p: give_back(p, p).wait_recv())
    out_ref[...] = returned[...]
    for g in range(GROUPS):
        others(g, lambda p: dispatch(p, s).wait_send())
        others(g, lambda p: give_back(p, s).wait_send())
        finish_sends(arrived, arrived_sems, g)
        finish_sends(hidden, hidden_sems, g)


GROUPS = 4


def grid_of(count):
    across = max(k for k in range(1, count + 1) if count % k == 0 and k * k <= count)
    return across, count // across


def through_experts(stream, gain, select, w_gate, w_up, w_down, n_sp, n_tp):
    count, cols = stream.shape
    slots = select.shape[0]
    width, units = w_gate.shape[1:]
    bf16, f32 = jnp.bfloat16, jnp.float32
    dma = pltpu.SemaphoreType.DMA
    across, down = grid_of(n_tp)
    straights, relays = across + down - 2, (across - 1) * (down - 1)
    vmem = pl.BlockSpec(memory_space=pltpu.VMEM)
    hbm = pl.BlockSpec(memory_space=pl.ANY)
    return pl.pallas_call(
        experts_kernel,
        out_shape=jax.ShapeDtypeStruct((slots, cols), bf16),
        in_specs=[vmem] * 3 + [hbm] * 3,
        out_specs=vmem,
        scratch_shapes=[
            pltpu.VMEM((width, units), bf16),
            pltpu.VMEM((width, units), bf16),
            pltpu.VMEM(w_down.shape[1:], bf16),
            pltpu.VMEM((n_tp, count, 128), f32),
            pltpu.VMEM((slots, cols), bf16),
            pltpu.VMEM((n_tp, slots, cols), bf16),
            pltpu.VMEM((n_tp, slots, units), bf16),
            pltpu.VMEM((slots, cols), bf16),
            pltpu.VMEM((slots, cols), bf16),
            pltpu.VMEM((slots // GROUPS, units), f32),
            pltpu.VMEM((slots // GROUPS, units), f32),
            pltpu.VMEM((slots // GROUPS, cols), f32),
            dma((3,)),
            dma((n_tp,)),
            dma((n_tp,)),
            dma((n_sp,)),
            dma((n_sp,)),
            dma((GROUPS, straights)),
            dma((GROUPS, n_tp)),
            dma((GROUPS, 2, relays)),
            dma((GROUPS, n_tp, 2)),
            dma((GROUPS, straights)),
            dma((GROUPS, n_tp)),
            dma((GROUPS, 2, relays)),
            dma((GROUPS, n_tp, 2)),
            dma((n_sp,)),
            dma((n_sp,)),
        ],
        compiler_params=pltpu.CompilerParams(
            collective_id=2, has_side_effects=True, vmem_limit_bytes=50 * 2**20
        ),
    )(stream, gain, select, w_gate, w_up, w_down)


def rotate(block, positions):
    half_dim = block.shape[-1] // 2
    inverse = jnp.power(THETA, -jnp.arange(half_dim, dtype=jnp.float32) * 2.0 / block.shape[-1])
    angles = positions[:, None, None] * inverse
    cosine_val, sine_val = (jnp.cos(angles), jnp.sin(angles))
    lower_half, upper_half = (block[..., :half_dim], block[..., half_dim:])
    return jnp.concatenate(
        [
            lower_half * cosine_val - upper_half * sine_val,
            upper_half * cosine_val + lower_half * sine_val,
        ],
        axis=-1,
    )


def block_terms(rot_queries, rot_keys, value_heads, rates):
    count = rates.shape[0]
    decay_sum = jnp.cumsum(rates, axis=0)
    by_head = decay_sum.T
    causal = (jnp.arange(count)[:, None] >= jnp.arange(count)[None, :])[None]
    spread = by_head[:, :, None] - by_head[:, None, :]
    weight = jnp.where(causal, jnp.exp(jnp.where(causal, spread, 0.0)), 0.0)
    scores = jnp.einsum("ihd,jhd->hij", rot_queries, rot_keys, preferred_element_type=jnp.float32)
    weighted = (scores * weight).astype(jnp.bfloat16)
    within = jnp.einsum("hij,jhv->ihv", weighted, value_heads, preferred_element_type=jnp.float32)
    block_end = decay_sum[-1]
    carried = (
        rot_keys.astype(jnp.float32) * jnp.exp(block_end[None, :] - decay_sum)[:, :, None]
    ).astype(jnp.bfloat16)
    update = jnp.einsum("jhd,jhv->hdv", carried, value_heads, preferred_element_type=jnp.float32)
    return (within, decay_sum, jnp.exp(block_end), update)


def final_result(rot_queries, decay_sum, within, state_in, gate_part, gain_part):
    cross_part = (
        jnp.einsum(
            "ihd,hdv->ihv",
            rot_queries,
            state_in,
            preferred_element_type=jnp.float32,
        )
        * jnp.exp(decay_sum)[:, :, None]
    )
    retained = within + cross_part
    scaled = retained * lax.rsqrt(jnp.mean(retained * retained, axis=-1, keepdims=True) + EPS)
    count, head_count, value_size = retained.shape
    gated = jax.nn.silu(gate_part.astype(jnp.float32)).reshape(count, head_count, value_size)
    return (
        (scaled * gain_part.reshape(head_count, value_size) * gated)
        .reshape(count, -1)
        .astype(jnp.bfloat16)
    )


def prepare(queries, keys_in, value_part, positions, head_count):
    row_count = queries.shape[0]
    key_size = queries.shape[1] // head_count
    rot_queries = rotate(
        queries.astype(jnp.float32).reshape(row_count, head_count, key_size), positions
    ).astype(jnp.bfloat16)
    rot_keys = (
        rotate(keys_in.astype(jnp.float32).reshape(row_count, head_count, key_size), positions)
        * key_size ** (-0.5)
    ).astype(jnp.bfloat16)
    value_heads = value_part.reshape(row_count, head_count, value_part.shape[1] // head_count)
    return (rot_queries, rot_keys, value_heads)


def per_device(
    residual,
    query_small,
    key_narrow_group,
    query_large,
    key_large,
    values,
    gates,
    log_decay,
    head_gain,
    out_weight,
    norm_gain,
    routes,
    route_weight,
    expert_gate,
    expert_up,
    expert_down,
):
    row_count = residual.shape[0]
    head_count = log_decay.shape[2]
    positions = (lax.axis_index("sp") * row_count + jnp.arange(row_count, dtype=jnp.int32)).astype(
        jnp.float32
    )
    query_a, key_a, value_a = prepare(
        query_small, key_narrow_group, values[:, 0], positions, head_count
    )
    query_b, key_b, value_b = prepare(query_large, key_large, values[:, 1], positions, head_count)
    within_a, decay_sum_a, fall_a, update_a = block_terms(query_a, key_a, value_a, log_decay[:, 0])
    within_b, decay_sum_b, fall_b, update_b = block_terms(query_b, key_b, value_b, log_decay[:, 1])

    n_sp, n_tp = lax.axis_size("sp"), lax.axis_size("tp")
    value_size = update_a.shape[2]
    piece = update_a.shape[1]
    parts = update_b.shape[1] // piece
    update = jnp.concatenate([update_a, update_b.reshape(-1, piece, value_size)], axis=0)
    fall = jnp.concatenate([fall_a, jnp.repeat(fall_b, parts)])
    fall = jnp.broadcast_to(fall[:, None, None], (fall.shape[0], 1, value_size))
    entering = entering_states(update, fall)
    state_a = entering[:head_count]
    state_b = entering[head_count:].reshape(update_b.shape)
    output_a = final_result(query_a, decay_sum_a, within_a, state_a, gates[:, 0], head_gain[0])
    output_b = final_result(query_b, decay_sum_b, within_b, state_b, gates[:, 1], head_gain[1])
    gathered = gather_heads(jnp.stack([output_a, output_b], axis=0), n_tp)
    weight = lax.all_gather(out_weight, "sp", axis=1, tiled=True)
    mixed = (
        jnp.dot(gathered[0], weight[0], preferred_element_type=jnp.float32)
        + jnp.dot(gathered[1], weight[1], preferred_element_type=jnp.float32)
    ).astype(jnp.bfloat16)
    stream = residual.astype(jnp.float32) + mixed.astype(jnp.float32)
    experts = lax.axis_size("sp")
    capacity = 4 * row_count // experts
    one_hot = (routes[:, :, None] == jnp.arange(experts, dtype=jnp.int32)[None, None, :]).astype(
        jnp.int32
    )
    one_hot = one_hot.reshape(2 * row_count, experts)
    before = jnp.cumsum(one_hot, axis=0) - one_hot
    slot_index = jnp.sum(before * one_hot, axis=1).reshape(row_count, 2)
    target = routes * capacity + slot_index
    slot_ids = jnp.arange(experts * capacity, dtype=jnp.int32)
    choose = target[:, :, None] == slot_ids[None, None, :]
    select = jnp.sum(choose.astype(jnp.int32), axis=1).astype(jnp.bfloat16).T
    returned = through_experts(
        stream, norm_gain[None, :], select, expert_gate, expert_up, expert_down, n_sp, n_tp
    )
    first_pick = jnp.dot(
        choose[:, 0].astype(jnp.bfloat16), returned, preferred_element_type=jnp.float32
    )
    second_pick = jnp.dot(
        choose[:, 1].astype(jnp.bfloat16), returned, preferred_element_type=jnp.float32
    )
    routed = route_weight[:, 0:1] * first_pick + route_weight[:, 1:2] * second_pick
    return (stream + routed).astype(jnp.bfloat16)


def solution(mesh):
    placed = (
        P("sp", "tp"),
        P("sp", "tp"),
        P("sp", "tp"),
        P("sp", "tp"),
        P("sp", "tp"),
        P("sp", None, "tp"),
        P("sp", None, "tp"),
        P("sp", None, "tp"),
        P(None, "tp"),
        P(None, "sp", "tp"),
        P("tp"),
        P("sp", None),
        P("sp", None),
        P("sp", None, "tp"),
        P("sp", None, "tp"),
        P("sp", None, "tp"),
    )
    return jax.shard_map(
        per_device, mesh=mesh, in_specs=placed, out_specs=P("sp", "tp"), check_vma=False
    )
```
